32 devices in a mesh: sp: 8 (over z, y), tp: 4 (over x, core).
Axes of the slice: x: 2, y: 2, z: 4, core: 2. Of those that a mesh axis runs over, the one named last changes fastest.
Arguments:
- tokens: bfloat16 [4096, 2048], P(('sp', 'tp')), may hold values from -6 to 6
- norm_gain: float32 [2048], replicated, may hold values from 0.1 to 1.9
- query_weight: bfloat16 [2048, 2048], P('sp', 'tp'), may hold values from -0.125 to 0.125
- key_weight: bfloat16 [2048, 2048], P('sp', 'tp'), may hold values from -0.125 to 0.125
- value_weight: bfloat16 [2048, 4096], P('sp', 'tp'), may hold values from -0.125 to 0.125
- retain_gate: bfloat16 [2048, 4096], P('sp', 'tp'), may hold values from -0.125 to 0.125
- unit_value: bfloat16 [2048, 2048], P('sp', 'tp'), may hold values from -0.125 to 0.125
- unit_gate: bfloat16 [2048, 2048], P('sp', 'tp'), may hold values from -0.125 to 0.125
- convolve_gate: bfloat16 [2048, 2048], P('sp', 'tp'), may hold values from -0.125 to 0.125
- filter_taps: float32 [31, 2048], replicated, may hold values from -1 to 1
- layer_gain: float32 [2048], replicated, may hold values from 0.1 to 1.9
- layer_shift: float32 [2048], replicated, may hold values from -3 to 3
- retain_output: bfloat16 [2048, 4096], P('sp', 'tp'), may hold values from -0.09375 to 0.09375
- convolve_output: bfloat16 [2048, 2048], P('sp', 'tp'), may hold values from -0.125 to 0.125
Outputs:
- mixed: bfloat16 [4096, 2048], P(('sp', 'tp'))
The draws below stay inside these ranges and needn't reach their ends.
All inputs are finite; a program needn't handle non-finite values.
Results may differ from the reference program's by a relative error of at most 0.018.
Values may be sent and summed in bfloat16 or wider, within the bound.
No kernel may reach another device: no remote copies, remote signals or barrier semaphores. Data moves between devices by JAX's collectives and lax.ppermute only.
A program may use at most 128 MiB of HBM per device.

```python
import jax
import jax.numpy as jnp
from jax import lax

D = 2048
HEADS = 8
KEY = 256
VAL = 512
CONV = 2048
GROUP = 512
KW = 31
TOK_DEV = 512
QK = 2048
VW = 4096
SEQ = 4096


def steps_of(stream_key, shape, cuts, smallest, top_value):
    gain, own = 1.0, jax.random.fold_in(stream_key, 6)
    for dim, shards_of in cuts:
        draws = jnp.exp(jax.random.uniform(jax.random.fold_in(own, dim), (shards_of,), jnp.float32, smallest / len(cuts), top_value / len(cuts)))
        gain = gain * jnp.repeat(draws, shape[dim] // shards_of).reshape([-1 if axis == dim else 1 for axis in range(len(shape))])
    return gain


def centred(own_key, extent, scale, most, shards=(), kind=jnp.bfloat16):
    drawn = jax.random.normal(own_key, extent, jnp.float32) * scale
    if len(shards) > 0:
        drawn = steps_of(own_key, extent, shards, -0.22, 0.18) * drawn
    return jnp.clip(drawn, min=-most, max=most).astype(kind)


def setup_inputs(seed: int = 0) -> dict:
    keys = jax.random.split(jax.random.key(seed), 15)
    return {
        "tokens": centred(keys[0], (SEQ, D), 1.0, 6.0, ((0, 32),)),
        "norm_gain": jnp.clip(1.0 + 0.18 * jax.random.normal(keys[1], (D,), jnp.float32), 0.1, 1.9),
        "query_weight": centred(keys[2], (D, QK), D ** -0.5, 0.125, ((0, 8), (1, 4))),
        "key_weight": centred(keys[3], (D, QK), D ** -0.5, 0.125, ((0, 8), (1, 4))),
        "value_weight": centred(keys[4], (D, VW), D ** -0.5, 0.125, ((0, 8), (1, 4))),
        "retain_gate": centred(keys[5], (D, VW), D ** -0.5, 0.125, ((0, 8), (1, 4))),
        "unit_value": centred(keys[6], (D, CONV), D ** -0.5, 0.125, ((0, 8), (1, 4))),
        "unit_gate": centred(keys[7], (D, CONV), D ** -0.5, 0.125, ((0, 8), (1, 4))),
        "convolve_gate": centred(keys[8], (D, CONV), D ** -0.5, 0.125, ((0, 8), (1, 4))),
        "filter_taps": centred(keys[9], (KW, CONV), KW ** -0.5, 1.0, (), jnp.float32),
        "layer_gain": jnp.clip(1.0 + 0.18 * jax.random.normal(keys[10], (CONV,), jnp.float32), 0.1, 1.9),
        "layer_shift": centred(keys[11], (CONV,), 0.5, 3.0, (), jnp.float32),
        "retain_output": centred(keys[12], (D, VW), VW ** -0.5, 0.09375, ((0, 8), (1, 4))),
        "convolve_output": centred(keys[13], (D, CONV), CONV ** -0.5, 0.125, ((0, 8), (1, 4))),
    }


rms_eps = 1e-06
group_eps = 1.0
layer_eps = 0.001
rope_base = 10000.0
highest = lax.Precision.HIGHEST

def rms_normalize(tokens, norm_gain):
    widened = tokens.astype(jnp.float32)
    scaled = widened * lax.rsqrt(lax.optimization_barrier(jnp.mean(widened * widened, axis=-1, keepdims=True)) + rms_eps)
    return (scaled * norm_gain).astype(jnp.bfloat16)

def widen(narrow_value):
    return lax.optimization_barrier(narrow_value.astype(jnp.bfloat16)).astype(jnp.float32)

def rotate(vectors, positions):
    half_width = vectors.shape[-1] // 2
    frequency = rope_base ** (-jnp.arange(half_width, dtype=jnp.float32) / half_width)
    angles = positions.astype(jnp.float32)[:, None] * frequency
    cosine = jnp.cos(angles)[:, None, :]
    sine_part = jnp.sin(angles)[:, None, :]
    front_half = vectors[..., :half_width]
    back_half = vectors[..., half_width:]
    return jnp.concatenate([front_half * cosine - back_half * sine_part, front_half * sine_part + back_half * cosine], axis=-1)

def prepare(queries, key_rows, values, positions):
    row_count = queries.shape[0]
    rotated_query = widen(rotate(queries.astype(jnp.float32).reshape(row_count, -1, KEY), positions))
    rotated_keys = widen(rotate(key_rows.astype(jnp.float32).reshape(row_count, -1, KEY), positions) * KEY ** (-0.5))
    value_heads = values.astype(jnp.float32).reshape(row_count, -1, VAL)
    return (rotated_query, rotated_keys, value_heads)

def decay_logs(first_head, head_total, all_heads, seq_length):
    ratio = (first_head + jnp.arange(head_total)).astype(jnp.float32) / (all_heads - 1)
    return (jnp.log(0.05) + ratio * jnp.log(18.0)) / seq_length

def local_parts(queries, key_rows, values, log_decay):
    row_count = queries.shape[0]
    indices = jnp.arange(row_count, dtype=jnp.float32)
    offsets = indices[:, None] - indices[None, :]
    causal = offsets >= 0
    weight = jnp.where(causal[None], jnp.exp(log_decay[:, None, None] * jnp.where(causal, offsets, 0.0)[None]), 0.0)
    scores = widen(jnp.einsum('ihd,jhd->hij', queries, key_rows) * weight)
    within = jnp.einsum('hij,jhe->ihe', scores, values)
    trailing = jnp.exp(log_decay[None, :] * (row_count - 1.0 - indices)[:, None])
    weighted = widen(key_rows * trailing[:, :, None])
    contribution = jnp.einsum('jhd,jhe->hde', weighted, values)
    return (within, contribution)

def cross_part(queries, carry_state, log_decay):
    row_count = queries.shape[0]
    indices = jnp.arange(row_count, dtype=jnp.float32)
    leading = jnp.exp(log_decay[None, :] * (indices + 1.0)[:, None])
    return jnp.einsum('ihd,hde->ihe', queries, carry_state, precision=highest) * leading[:, :, None]

def retain_finish(raw, switch):
    average = lax.optimization_barrier(jnp.mean(raw, axis=-1, keepdims=True))
    spread = lax.optimization_barrier(jnp.mean(jnp.square(raw - average), axis=-1, keepdims=True))
    normalized = ((raw - average) * lax.rsqrt(spread + group_eps)).reshape(raw.shape[0], -1)
    return (normalized * jax.nn.silu(switch.astype(jnp.float32))).astype(jnp.bfloat16)

def convolve_branch(gated_input, before, tap_slice, gain_slice, shift_slice, switch):
    padded = jnp.concatenate([before, gated_input], axis=0)
    row_count = gated_input.shape[0]
    summed = jnp.zeros(gated_input.shape, jnp.float32)
    for tap_index in range(tap_slice.shape[0]):
        summed = summed + padded[tap_index:tap_index + row_count].astype(jnp.float32) * tap_slice[tap_index]
    grouped = summed.reshape(row_count, -1, GROUP)
    average = lax.optimization_barrier(jnp.mean(grouped, axis=-1, keepdims=True))
    spread = lax.optimization_barrier(jnp.mean(jnp.square(grouped - average), axis=-1, keepdims=True))
    normalized = ((grouped - average) * lax.rsqrt(spread + layer_eps)).reshape(row_count, -1)
    normalized = normalized * gain_slice + shift_slice
    return (jax.nn.silu(normalized) * jax.nn.silu(switch.astype(jnp.float32))).astype(jnp.bfloat16)

def contract(hidden, matrix):
    return lax.dot_general(hidden, matrix, (((1,), (1,)), ((), ())), preferred_element_type=jnp.float32)

def reference(tokens, norm_gain, query_weight, key_weight, value_weight, retain_gate, unit_value, unit_gate, convolve_gate, filter_taps, layer_gain, layer_shift, retain_output, convolve_output):
    seq_total = tokens.shape[0]
    normed = rms_normalize(tokens, norm_gain)

    def project(matrix):
        return jnp.dot(normed, matrix, preferred_element_type=jnp.float32).astype(jnp.bfloat16)
    queries = project(query_weight)
    key_rows = project(key_weight)
    values = project(value_weight)
    retain_switch = project(retain_gate)
    glu_value = project(unit_value)
    glu_switch = project(unit_gate)
    convolve_switch = project(convolve_gate)
    positions = jnp.arange(seq_total, dtype=jnp.int32)
    rotated_query, rotated_keys, value_heads = prepare(queries, key_rows, values, positions)
    log_decay = decay_logs(0, HEADS, HEADS, seq_total)
    totals = jnp.exp(log_decay * TOK_DEV)
    blocks = seq_total // TOK_DEV

    def advance(carry_state, block):
        block_query, block_keys, block_values = block
        within, contribution = local_parts(block_query, block_keys, block_values, log_decay)
        result = within + cross_part(block_query, carry_state, log_decay)
        return (carry_state * totals[:, None, None] + contribution, result)
    start_state = jnp.zeros((HEADS, KEY, VAL), jnp.float32)
    final_state, outputs = lax.scan(advance, start_state, (rotated_query.reshape(blocks, TOK_DEV, HEADS, KEY), rotated_keys.reshape(blocks, TOK_DEV, HEADS, KEY), value_heads.reshape(blocks, TOK_DEV, HEADS, VAL)))
    raw = outputs.reshape(seq_total, HEADS, VAL)
    retain_hidden = retain_finish(raw, retain_switch)
    gated_input = (glu_value.astype(jnp.float32) * jax.nn.sigmoid(glu_switch.astype(jnp.float32))).astype(jnp.bfloat16)
    before = jnp.zeros((KW - 1, CONV), jnp.bfloat16)
    convolve_hidden = convolve_branch(gated_input, before, filter_taps, layer_gain, layer_shift, convolve_switch)
    summed = contract(retain_hidden, retain_output) + contract(convolve_hidden, convolve_output)
    return summed.astype(jnp.bfloat16)
```

```python
import jax
import jax.numpy as jnp
from jax import lax
from jax.sharding import PartitionSpec as P

KEY = 256
VAL = 512
GROUP = 512
KW = 31


rms_eps = 1e-06
group_eps = 1.0
layer_eps = 0.001
rope_base = 10000.0


def from_behind(x, axis, by):
    length = lax.axis_size(axis)
    pairs = [(i, i + by) for i in range(length) if 0 <= i + by < length]
    return lax.ppermute(x, axis, pairs)


def partners(axis, bit):
    return [(i, i ^ bit) for i in range(lax.axis_size(axis))]


def gather_rows(x, axis):
    rank = lax.axis_index(axis)
    blocks = x[None]
    bit = lax.axis_size(axis) // 2
    while bit >= 1:
        other = lax.ppermute(blocks, axis, partners(axis, bit))
        low = (rank & bit) == 0
        blocks = jnp.stack(
            [jnp.where(low, blocks, other), jnp.where(low, other, blocks)], axis=1
        ).reshape((-1,) + x.shape)
        bit //= 2
    return blocks.reshape((-1,) + x.shape[1:])


def scatter_sums(make, hidden, axis):
    size = lax.axis_size(axis)
    rank = lax.axis_index(axis)
    rows = hidden.shape[0] // size
    parity = rank & 1
    paired = hidden.reshape(size // 2, 2, rows, hidden.shape[1])

    def half(which):
        taken = lax.dynamic_index_in_dim(paired, which, 1, False)
        return make(taken.reshape(-1, hidden.shape[1])).reshape(size // 2, rows, -1)

    away = half(1 - parity).astype(jnp.bfloat16)
    arrived = lax.ppermute(away, axis, partners(axis, 1))
    total = half(parity) + arrived.astype(jnp.float32)
    bit = 2
    while bit < size:
        mine = (rank // bit) & 1
        split = total.reshape(-1, 2, rows, total.shape[-1])
        away = lax.dynamic_index_in_dim(split, 1 - mine, 1, False).astype(jnp.bfloat16)
        arrived = lax.ppermute(away, axis, partners(axis, bit))
        total = lax.dynamic_index_in_dim(split, mine, 1, False) + arrived.astype(jnp.float32)
        bit *= 2
    return total.reshape(rows, -1).astype(jnp.bfloat16)


def state_before(contribution, totals, axis):
    size = lax.axis_size(axis)
    carried = from_behind(contribution.astype(jnp.bfloat16), axis, 1).astype(jnp.float32)
    decay = totals
    reach = 1
    while reach < size - 1:
        earlier = from_behind(carried.astype(jnp.bfloat16), axis, reach).astype(jnp.float32)
        carried = carried + decay[:, None, None] * earlier
        decay = decay * decay
        reach *= 2
    return carried


def rms_normalize(tokens, norm_gain):
    widened = tokens.astype(jnp.float32)
    scaled = widened * lax.rsqrt(jnp.mean(widened * widened, axis=-1, keepdims=True) + rms_eps)
    return (scaled * norm_gain).astype(jnp.bfloat16)


def rotate(vectors, positions):
    half_width = vectors.shape[-1] // 2
    frequency = rope_base ** (-jnp.arange(half_width, dtype=jnp.float32) / half_width)
    angles = positions.astype(jnp.float32)[:, None] * frequency
    cosine = jnp.cos(angles)[:, None, :]
    sine_part = jnp.sin(angles)[:, None, :]
    front_half = vectors[..., :half_width]
    back_half = vectors[..., half_width:]
    return jnp.concatenate(
        [front_half * cosine - back_half * sine_part, front_half * sine_part + back_half * cosine],
        axis=-1,
    )


def prepare(queries, key_rows, values, positions):
    row_count = queries.shape[0]
    rotated_query = rotate(
        queries.astype(jnp.float32).reshape(row_count, -1, KEY), positions
    ).astype(jnp.bfloat16)
    rotated_keys = (
        rotate(key_rows.astype(jnp.float32).reshape(row_count, -1, KEY), positions) * KEY ** (-0.5)
    ).astype(jnp.bfloat16)
    value_heads = values.reshape(row_count, -1, VAL)
    return (rotated_query, rotated_keys, value_heads)


def decay_logs(first_head, head_total, all_heads, seq_length):
    ratio = (first_head + jnp.arange(head_total)).astype(jnp.float32) / (all_heads - 1)
    return (jnp.log(0.05) + ratio * jnp.log(18.0)) / seq_length


def local_parts(queries, key_rows, values, log_decay):
    row_count = queries.shape[0]
    indices = jnp.arange(row_count, dtype=jnp.float32)
    offsets = indices[:, None] - indices[None, :]
    causal = offsets >= 0
    weight = jnp.where(
        causal[None], jnp.exp(log_decay[:, None, None] * jnp.where(causal, offsets, 0.0)[None]), 0.0
    )
    scores = (
        jnp.einsum("ihd,jhd->hij", queries, key_rows, preferred_element_type=jnp.float32) * weight
    ).astype(jnp.bfloat16)
    within = jnp.einsum("hij,jhe->ihe", scores, values, preferred_element_type=jnp.float32)
    trailing = jnp.exp(log_decay[None, :] * (row_count - 1.0 - indices)[:, None])
    weighted = (key_rows.astype(jnp.float32) * trailing[:, :, None]).astype(jnp.bfloat16)
    contribution = jnp.einsum("jhd,jhe->hde", weighted, values, preferred_element_type=jnp.float32)
    return (within, contribution)


def cross_part(queries, carry_state, log_decay):
    row_count = queries.shape[0]
    indices = jnp.arange(row_count, dtype=jnp.float32)
    leading = jnp.exp(log_decay[None, :] * (indices + 1.0)[:, None])
    return (
        jnp.einsum(
            "ihd,hde->ihe",
            queries,
            carry_state.astype(jnp.bfloat16),
            preferred_element_type=jnp.float32,
        )
        * leading[:, :, None]
    )


def retain_finish(raw, switch):
    average = jnp.mean(raw, axis=-1, keepdims=True)
    spread = jnp.mean(jnp.square(raw - average), axis=-1, keepdims=True)
    normalized = ((raw - average) * lax.rsqrt(spread + group_eps)).reshape(raw.shape[0], -1)
    return (normalized * jax.nn.silu(switch.astype(jnp.float32))).astype(jnp.bfloat16)


def convolve_branch(gated_input, before, tap_slice, gain_slice, shift_slice, switch):
    padded = jnp.concatenate([before, gated_input], axis=0)
    row_count = gated_input.shape[0]
    summed = jnp.zeros(gated_input.shape, jnp.float32)
    for tap_index in range(tap_slice.shape[0]):
        summed = (
            summed
            + padded[tap_index : tap_index + row_count].astype(jnp.float32) * tap_slice[tap_index]
        )
    grouped = summed.reshape(row_count, -1, GROUP)
    average = jnp.mean(grouped, axis=-1, keepdims=True)
    spread = jnp.mean(jnp.square(grouped - average), axis=-1, keepdims=True)
    normalized = ((grouped - average) * lax.rsqrt(spread + layer_eps)).reshape(row_count, -1)
    normalized = normalized * gain_slice + shift_slice
    return (jax.nn.silu(normalized) * jax.nn.silu(switch.astype(jnp.float32))).astype(jnp.bfloat16)


def contract(hidden, matrix):
    return lax.dot_general(
        hidden, matrix, (((1,), (1,)), ((), ())), preferred_element_type=jnp.float32
    )


def local(
    tokens,
    norm_gain,
    query_weight,
    key_weight,
    value_weight,
    retain_gate,
    unit_value,
    unit_gate,
    convolve_gate,
    filter_taps,
    layer_gain,
    layer_shift,
    retain_output,
    convolve_output,
):
    head_groups = lax.axis_size("tp")
    chain_length = lax.axis_size("sp")
    head_rank = lax.axis_index("tp")
    chain_rank = lax.axis_index("sp")
    normed = rms_normalize(tokens, norm_gain)
    in_weights = (
        query_weight,
        key_weight,
        value_weight,
        retain_gate,
        unit_value,
        unit_gate,
        convolve_gate,
    )
    in_full = lax.all_gather(jnp.concatenate(in_weights, axis=1), "sp", axis=0, tiled=True)
    out_full = lax.all_gather(
        jnp.concatenate((retain_output, convolve_output), axis=1), "sp", axis=0, tiled=True
    )
    rows = gather_rows(normed, "tp")
    row_count = rows.shape[0]
    projected = jnp.dot(rows, in_full, preferred_element_type=jnp.float32).astype(jnp.bfloat16)
    bounds = [0]
    for matrix in in_weights:
        bounds.append(bounds[-1] + matrix.shape[1])
    pieces = [projected[:, bounds[column] : bounds[column + 1]] for column in range(7)]
    queries, key_rows, values, retain_switch, glu_value, glu_switch, convolve_switch = pieces
    local_heads = queries.shape[1] // KEY
    positions = chain_rank * row_count + jnp.arange(row_count, dtype=jnp.int32)
    rotated_query, rotated_keys, value_heads = prepare(queries, key_rows, values, positions)
    log_decay = decay_logs(
        head_rank * local_heads, local_heads, local_heads * head_groups, row_count * chain_length
    )
    within, contribution = local_parts(rotated_query, rotated_keys, value_heads, log_decay)
    totals = jnp.exp(log_decay * row_count)
    gated_input = (
        glu_value.astype(jnp.float32) * jax.nn.sigmoid(glu_switch.astype(jnp.float32))
    ).astype(jnp.bfloat16)
    channels = gated_input.shape[1]
    before = from_behind(gated_input[row_count - (KW - 1) :], "sp", 1)
    incoming = state_before(contribution, totals, "sp")
    raw = within + cross_part(rotated_query, incoming, log_decay)
    retain_hidden = retain_finish(raw, retain_switch)
    tap_slice = lax.dynamic_slice_in_dim(filter_taps, head_rank * channels, channels, 1)
    gain_slice = lax.dynamic_slice_in_dim(layer_gain, head_rank * channels, channels, 0)
    shift_slice = lax.dynamic_slice_in_dim(layer_shift, head_rank * channels, channels, 0)
    convolve_hidden = convolve_branch(
        gated_input, before, tap_slice, gain_slice, shift_slice, convolve_switch
    )
    hidden = jnp.concatenate((retain_hidden, convolve_hidden), axis=1)
    return scatter_sums(lambda rows: contract(rows, out_full), hidden, "tp")


def solution(mesh):
    return jax.shard_map(
        local,
        mesh=mesh,
        in_specs=(
            P(("sp", "tp"), None),
            P(),
            P("sp", "tp"),
            P("sp", "tp"),
            P("sp", "tp"),
            P("sp", "tp"),
            P("sp", "tp"),
            P("sp", "tp"),
            P("sp", "tp"),
            P(),
            P(),
            P(),
            P("sp", "tp"),
            P("sp", "tp"),
        ),
        out_specs=P(("sp", "tp"), None),
        check_vma=False,
    )
```

```python
import jax
import jax.numpy as jnp
from jax import lax
from jax.sharding import PartitionSpec as P

KEY = 256
VAL = 512
GROUP = 512
KW = 31


rms_eps = 1e-06
group_eps = 1.0
layer_eps = 0.001
rope_base = 10000.0


def from_behind(x, axis, by):
    length = lax.axis_size(axis)
    pairs = [(i, i + by) for i in range(length) if 0 <= i + by < length]
    return lax.ppermute(x, axis, pairs)


def partners(axis, bit):
    return [(i, i ^ bit) for i in range(lax.axis_size(axis))]


def gather_rows(x, axis):
    rank = lax.axis_index(axis)
    blocks = x[None]
    bit = lax.axis_size(axis) // 2
    while bit >= 1:
        other = lax.ppermute(blocks, axis, partners(axis, bit))
        low = (rank & bit) == 0
        blocks = jnp.stack(
            [jnp.where(low, blocks, other), jnp.where(low, other, blocks)], axis=1
        ).reshape((-1,) + x.shape)
        bit //= 2
    return blocks.reshape((-1,) + x.shape[1:])


def scatter_sums(make, hidden, axis):
    size = lax.axis_size(axis)
    rank = lax.axis_index(axis)
    rows = hidden.shape[0] // size
    parity = rank & 1
    paired = hidden.reshape(size // 2, 2, rows, hidden.shape[1])

    def half(which):
        taken = lax.dynamic_index_in_dim(paired, which, 1, False)
        return make(taken.reshape(-1, hidden.shape[1])).reshape(size // 2, rows, -1)

    away = half(1 - parity).astype(jnp.bfloat16)
    arrived = lax.ppermute(away, axis, partners(axis, 1))
    total = half(parity) + arrived.astype(jnp.float32)
    bit = 2
    while bit < size:
        mine = (rank // bit) & 1
        split = total.reshape(-1, 2, rows, total.shape[-1])
        away = lax.dynamic_index_in_dim(split, 1 - mine, 1, False).astype(jnp.bfloat16)
        arrived = lax.ppermute(away, axis, partners(axis, bit))
        total = lax.dynamic_index_in_dim(split, mine, 1, False) + arrived.astype(jnp.float32)
        bit *= 2
    return total.reshape(rows, -1).astype(jnp.bfloat16)


def state_before(contribution, totals, axis):
    size = lax.axis_size(axis)
    carried = from_behind(contribution.astype(jnp.bfloat16), axis, 1).astype(jnp.float32)
    decay = totals
    reach = 1
    while reach < size - 1:
        earlier = from_behind(carried.astype(jnp.bfloat16), axis, reach).astype(jnp.float32)
        carried = carried + decay[:, None, None] * earlier
        decay = decay * decay
        reach *= 2
    return carried


def rms_normalize(tokens, norm_gain):
    widened = tokens.astype(jnp.float32)
    scaled = widened * lax.rsqrt(jnp.mean(widened * widened, axis=-1, keepdims=True) + rms_eps)
    return (scaled * norm_gain).astype(jnp.bfloat16)


def rotate(vectors, positions):
    half_width = vectors.shape[-1] // 2
    frequency = rope_base ** (-jnp.arange(half_width, dtype=jnp.float32) / half_width)
    angles = positions.astype(jnp.float32)[:, None] * frequency
    cosine = jnp.cos(angles)[:, None, :]
    sine_part = jnp.sin(angles)[:, None, :]
    front_half = vectors[..., :half_width]
    back_half = vectors[..., half_width:]
    return jnp.concatenate(
        [front_half * cosine - back_half * sine_part, front_half * sine_part + back_half * cosine],
        axis=-1,
    )


def prepare(queries, key_rows, values, positions):
    row_count = queries.shape[0]
    rotated_query = rotate(
        queries.astype(jnp.float32).reshape(row_count, -1, KEY), positions
    ).astype(jnp.bfloat16)
    rotated_keys = (
        rotate(key_rows.astype(jnp.float32).reshape(row_count, -1, KEY), positions) * KEY ** (-0.5)
    ).astype(jnp.bfloat16)
    value_heads = values.reshape(row_count, -1, VAL)
    return (rotated_query, rotated_keys, value_heads)


def decay_logs(first_head, head_total, all_heads, seq_length):
    ratio = (first_head + jnp.arange(head_total)).astype(jnp.float32) / (all_heads - 1)
    return (jnp.log(0.05) + ratio * jnp.log(18.0)) / seq_length


def local_parts(queries, key_rows, values, log_decay):
    row_count = queries.shape[0]
    indices = jnp.arange(row_count, dtype=jnp.float32)
    offsets = indices[:, None] - indices[None, :]
    causal = offsets >= 0
    weight = jnp.where(
        causal[None], jnp.exp(log_decay[:, None, None] * jnp.where(causal, offsets, 0.0)[None]), 0.0
    )
    scores = (
        jnp.einsum("ihd,jhd->hij", queries, key_rows, preferred_element_type=jnp.float32) * weight
    ).astype(jnp.bfloat16)
    within = jnp.einsum("hij,jhe->ihe", scores, values, preferred_element_type=jnp.float32)
    trailing = jnp.exp(log_decay[None, :] * (row_count - 1.0 - indices)[:, None])
    weighted = (key_rows.astype(jnp.float32) * trailing[:, :, None]).astype(jnp.bfloat16)
    contribution = jnp.einsum("jhd,jhe->hde", weighted, values, preferred_element_type=jnp.float32)
    return (within, contribution)


def cross_part(queries, carry_state, log_decay):
    row_count = queries.shape[0]
    indices = jnp.arange(row_count, dtype=jnp.float32)
    leading = jnp.exp(log_decay[None, :] * (indices + 1.0)[:, None])
    return (
        jnp.einsum(
            "ihd,hde->ihe",
            queries,
            carry_state.astype(jnp.bfloat16),
            preferred_element_type=jnp.float32,
        )
        * leading[:, :, None]
    )


def retain_finish(raw, switch):
    average = jnp.mean(raw, axis=-1, keepdims=True)
    spread = jnp.mean(jnp.square(raw - average), axis=-1, keepdims=True)
    normalized = ((raw - average) * lax.rsqrt(spread + group_eps)).reshape(raw.shape[0], -1)
    return (normalized * jax.nn.silu(switch.astype(jnp.float32))).astype(jnp.bfloat16)


def convolve_branch(gated_input, before, tap_slice, gain_slice, shift_slice, switch):
    padded = jnp.concatenate([before, gated_input], axis=0)
    row_count = gated_input.shape[0]
    summed = jnp.zeros(gated_input.shape, jnp.float32)
    for tap_index in range(tap_slice.shape[0]):
        summed = (
            summed
            + padded[tap_index : tap_index + row_count].astype(jnp.float32) * tap_slice[tap_index]
        )
    grouped = summed.reshape(row_count, -1, GROUP)
    average = jnp.mean(grouped, axis=-1, keepdims=True)
    spread = jnp.mean(jnp.square(grouped - average), axis=-1, keepdims=True)
    normalized = ((grouped - average) * lax.rsqrt(spread + layer_eps)).reshape(row_count, -1)
    normalized = normalized * gain_slice + shift_slice
    return (jax.nn.silu(normalized) * jax.nn.silu(switch.astype(jnp.float32))).astype(jnp.bfloat16)


def contract(hidden, matrix):
    return lax.dot_general(
        hidden, matrix, (((1,), (1,)), ((), ())), preferred_element_type=jnp.float32
    )


def local(
    tokens,
    norm_gain,
    query_weight,
    key_weight,
    value_weight,
    retain_gate,
    unit_value,
    unit_gate,
    convolve_gate,
    filter_taps,
    layer_gain,
    layer_shift,
    retain_output,
    convolve_output,
):
    head_groups = lax.axis_size("tp")
    chain_length = lax.axis_size("sp")
    head_rank = lax.axis_index("tp")
    chain_rank = lax.axis_index("sp")
    normed = rms_normalize(tokens, norm_gain)
    in_weights = (
        query_weight,
        key_weight,
        value_weight,
        retain_gate,
        unit_value,
        unit_gate,
        convolve_gate,
    )
    def whole(*parts):
        packed = jnp.concatenate(parts, axis=1)
        return lax.all_gather(packed, "sp", axis=0, tiled=True)

    first = whole(*in_weights[:3])
    second = whole(*in_weights[3:6])
    third = whole(in_weights[6], retain_output, convolve_output)
    width = convolve_gate.shape[1]
    out_full = third[:, width:]
    rows = gather_rows(normed, "tp")
    row_count = rows.shape[0]

    def project(matrix, widths):
        made = jnp.dot(rows, matrix, preferred_element_type=jnp.float32).astype(jnp.bfloat16)
        bounds = [sum(widths[:i]) for i in range(len(widths) + 1)]
        return [made[:, bounds[i] : bounds[i + 1]] for i in range(len(widths))]

    widths = [matrix.shape[1] for matrix in in_weights]
    pieces = (
        project(first, widths[:3])
        + project(second, widths[3:6])
        + project(third[:, :width], widths[6:])
    )
    queries, key_rows, values, retain_switch, glu_value, glu_switch, convolve_switch = pieces
    local_heads = queries.shape[1] // KEY
    positions = chain_rank * row_count + jnp.arange(row_count, dtype=jnp.int32)
    rotated_query, rotated_keys, value_heads = prepare(queries, key_rows, values, positions)
    log_decay = decay_logs(
        head_rank * local_heads, local_heads, local_heads * head_groups, row_count * chain_length
    )
    within, contribution = local_parts(rotated_query, rotated_keys, value_heads, log_decay)
    totals = jnp.exp(log_decay * row_count)
    gated_input = (
        glu_value.astype(jnp.float32) * jax.nn.sigmoid(glu_switch.astype(jnp.float32))
    ).astype(jnp.bfloat16)
    channels = gated_input.shape[1]
    before = from_behind(gated_input[row_count - (KW - 1) :], "sp", 1)
    incoming = state_before(contribution, totals, "sp")
    raw = within + cross_part(rotated_query, incoming, log_decay)
    retain_hidden = retain_finish(raw, retain_switch)
    tap_slice = lax.dynamic_slice_in_dim(filter_taps, head_rank * channels, channels, 1)
    gain_slice = lax.dynamic_slice_in_dim(layer_gain, head_rank * channels, channels, 0)
    shift_slice = lax.dynamic_slice_in_dim(layer_shift, head_rank * channels, channels, 0)
    convolve_hidden = convolve_branch(
        gated_input, before, tap_slice, gain_slice, shift_slice, convolve_switch
    )
    hidden = jnp.concatenate((retain_hidden, convolve_hidden), axis=1)
    return scatter_sums(lambda rows: contract(rows, out_full), hidden, "tp")


def solution(mesh):
    return jax.shard_map(
        local,
        mesh=mesh,
        in_specs=(
            P(("sp", "tp"), None),
            P(),
            P("sp", "tp"),
            P("sp", "tp"),
            P("sp", "tp"),
            P("sp", "tp"),
            P("sp", "tp"),
            P("sp", "tp"),
            P("sp", "tp"),
            P(),
            P(),
            P(),
            P("sp", "tp"),
            P("sp", "tp"),
        ),
        out_specs=P(("sp", "tp"), None),
        check_vma=False,
    )
```

```python
import jax
import jax.numpy as jnp
from jax import lax
from jax.sharding import PartitionSpec as P

KEY = 256
VAL = 512
GROUP = 512
KW = 31


rms_eps = 1e-06
group_eps = 1.0
layer_eps = 0.001
rope_base = 10000.0


def from_behind(x, axis, by):
    length = lax.axis_size(axis)
    pairs = [(i, i + by) for i in range(length) if 0 <= i + by < length]
    return lax.ppermute(x, axis, pairs)


def partners(axis, bit):
    return [(i, i ^ bit) for i in range(lax.axis_size(axis))]


def gather_rows(x, axis):
    rank = lax.axis_index(axis)
    blocks = x[None]
    bit = lax.axis_size(axis) // 2
    while bit >= 1:
        other = lax.ppermute(blocks, axis, partners(axis, bit))
        low = (rank & bit) == 0
        blocks = jnp.stack(
            [jnp.where(low, blocks, other), jnp.where(low, other, blocks)], axis=1
        ).reshape((-1,) + x.shape)
        bit //= 2
    return blocks.reshape((-1,) + x.shape[1:])


def scatter_sums(make, hidden, axis, pair_axis):
    ranks = lax.axis_size(axis)
    rank = lax.axis_index(axis)
    size = 2 * ranks
    rows = hidden.shape[0] // size
    parity = rank & 1
    paired = hidden.reshape(size // 2, 2, rows, hidden.shape[1])

    def half(which):
        taken = lax.dynamic_index_in_dim(paired, which, 1, False)
        return make(taken.reshape(-1, hidden.shape[1])).reshape(size // 2, rows, -1)

    away = half(1 - parity).astype(jnp.bfloat16)
    arrived = lax.ppermute(away, axis, partners(axis, 1))
    total = half(parity) + arrived.astype(jnp.float32)
    bit = 2
    while bit < size:
        if bit < ranks:
            mine, name, hop = (rank // bit) & 1, axis, bit
        else:
            mine, name, hop = lax.axis_index(pair_axis) & 1, pair_axis, 1
        split = total.reshape(-1, 2, rows, total.shape[-1])
        away = lax.dynamic_index_in_dim(split, 1 - mine, 1, False).astype(jnp.bfloat16)
        arrived = lax.ppermute(away, name, partners(name, hop))
        total = lax.dynamic_index_in_dim(split, mine, 1, False) + arrived.astype(jnp.float32)
        bit *= 2
    return total.reshape(rows, -1).astype(jnp.bfloat16)


def state_before(contribution, totals, axis):
    size = lax.axis_size(axis) // 2
    carried = from_behind(contribution.astype(jnp.bfloat16), axis, 2).astype(jnp.float32)
    decay = totals
    reach = 1
    while reach < size - 1:
        earlier = from_behind(carried.astype(jnp.bfloat16), axis, 2 * reach).astype(jnp.float32)
        carried = carried + decay[:, None, None] * earlier
        decay = decay * decay
        reach *= 2
    return carried


def rms_normalize(tokens, norm_gain):
    widened = tokens.astype(jnp.float32)
    scaled = widened * lax.rsqrt(jnp.mean(widened * widened, axis=-1, keepdims=True) + rms_eps)
    return (scaled * norm_gain).astype(jnp.bfloat16)


def rotate(vectors, positions):
    half_width = vectors.shape[-1] // 2
    frequency = rope_base ** (-jnp.arange(half_width, dtype=jnp.float32) / half_width)
    angles = positions.astype(jnp.float32)[:, None] * frequency
    cosine = jnp.cos(angles)[:, None, :]
    sine_part = jnp.sin(angles)[:, None, :]
    front_half = vectors[..., :half_width]
    back_half = vectors[..., half_width:]
    return jnp.concatenate(
        [front_half * cosine - back_half * sine_part, front_half * sine_part + back_half * cosine],
        axis=-1,
    )


def prepare(queries, key_rows, values, positions):
    row_count = queries.shape[0]
    rotated_query = rotate(
        queries.astype(jnp.float32).reshape(row_count, -1, KEY), positions
    ).astype(jnp.bfloat16)
    rotated_keys = (
        rotate(key_rows.astype(jnp.float32).reshape(row_count, -1, KEY), positions) * KEY ** (-0.5)
    ).astype(jnp.bfloat16)
    value_heads = values.reshape(row_count, -1, VAL)
    return (rotated_query, rotated_keys, value_heads)


def decay_logs(first_head, head_total, all_heads, seq_length):
    ratio = (first_head + jnp.arange(head_total)).astype(jnp.float32) / (all_heads - 1)
    return (jnp.log(0.05) + ratio * jnp.log(18.0)) / seq_length


def local_parts(queries, key_rows, values, log_decay):
    row_count = queries.shape[0]
    indices = jnp.arange(row_count, dtype=jnp.float32)
    offsets = indices[:, None] - indices[None, :]
    causal = offsets >= 0
    weight = jnp.where(
        causal[None], jnp.exp(log_decay[:, None, None] * jnp.where(causal, offsets, 0.0)[None]), 0.0
    )
    scores = (
        jnp.einsum("ihd,jhd->hij", queries, key_rows, preferred_element_type=jnp.float32) * weight
    ).astype(jnp.bfloat16)
    within = jnp.einsum("hij,jhe->ihe", scores, values, preferred_element_type=jnp.float32)
    trailing = jnp.exp(log_decay[None, :] * (row_count - 1.0 - indices)[:, None])
    weighted = (key_rows.astype(jnp.float32) * trailing[:, :, None]).astype(jnp.bfloat16)
    contribution = jnp.einsum("jhd,jhe->hde", weighted, values, preferred_element_type=jnp.float32)
    return (within, contribution)


def cross_part(queries, carry_state, log_decay):
    row_count = queries.shape[0]
    indices = jnp.arange(row_count, dtype=jnp.float32)
    leading = jnp.exp(log_decay[None, :] * (indices + 1.0)[:, None])
    return (
        jnp.einsum(
            "ihd,hde->ihe",
            queries,
            carry_state.astype(jnp.bfloat16),
            preferred_element_type=jnp.float32,
        )
        * leading[:, :, None]
    )


def retain_finish(raw, switch):
    average = jnp.mean(raw, axis=-1, keepdims=True)
    spread = jnp.mean(jnp.square(raw - average), axis=-1, keepdims=True)
    normalized = ((raw - average) * lax.rsqrt(spread + group_eps)).reshape(raw.shape[0], -1)
    return (normalized * jax.nn.silu(switch.astype(jnp.float32))).astype(jnp.bfloat16)


def convolve_branch(gated_input, before, tap_slice, gain_slice, shift_slice, switch):
    padded = jnp.concatenate([before, gated_input], axis=0)
    row_count = gated_input.shape[0]
    summed = jnp.zeros(gated_input.shape, jnp.float32)
    for tap_index in range(tap_slice.shape[0]):
        summed = (
            summed
            + padded[tap_index : tap_index + row_count].astype(jnp.float32) * tap_slice[tap_index]
        )
    def group_mean(x):
        own = jnp.sum(x, axis=-1)
        other = lax.ppermute(own, "sp", partners("sp", 1))
        return ((own + other) / (2 * x.shape[1]))[:, None]

    average = group_mean(summed)
    spread = group_mean(jnp.square(summed - average))
    normalized = (summed - average) * lax.rsqrt(spread + layer_eps)
    normalized = normalized * gain_slice + shift_slice
    return (jax.nn.silu(normalized) * jax.nn.silu(switch.astype(jnp.float32))).astype(jnp.bfloat16)


def contract(hidden, matrix):
    return lax.dot_general(
        hidden, matrix, (((1,), (1,)), ((), ())), preferred_element_type=jnp.float32
    )


def local(
    tokens,
    norm_gain,
    query_weight,
    key_weight,
    value_weight,
    retain_gate,
    unit_value,
    unit_gate,
    convolve_gate,
    filter_taps,
    layer_gain,
    layer_shift,
    retain_output,
    convolve_output,
):
    head_groups = lax.axis_size("tp")
    chain_length = lax.axis_size("sp")
    head_rank = lax.axis_index("tp")
    chain_rank = lax.axis_index("sp")
    normed = rms_normalize(tokens, norm_gain)
    side = chain_rank & 1
    pairs_total = chain_length // 2
    lines = [[i for i in range(chain_length) if i % 2 == j] for j in range(2)]

    def of_pair(own):
        other = lax.ppermute(own, "sp", partners("sp", 1))
        low = side == 0
        return jnp.concatenate([jnp.where(low, own, other), jnp.where(low, other, own)], axis=0)

    def whole(*parts):
        def packed(which):
            return jnp.concatenate(
                [
                    lax.dynamic_slice_in_dim(m, which * (m.shape[1] // 2), m.shape[1] // 2, 1)
                    for m in parts
                ],
                axis=1,
            )

        kept = packed(side)
        arrived = lax.ppermute(packed(1 - side), "sp", partners("sp", 1))
        low = side == 0
        both = jnp.concatenate(
            [jnp.where(low, kept, arrived), jnp.where(low, arrived, kept)], axis=0
        )
        return lax.all_gather(both, "sp", axis=0, tiled=True, axis_index_groups=lines)

    first = whole(query_weight, key_weight, value_weight, unit_value, unit_gate)
    second = whole(retain_gate, convolve_gate, retain_output, convolve_output)
    rows = gather_rows(of_pair(normed), "tp")
    rows = rows.reshape(head_groups, 2, -1, rows.shape[1]).swapaxes(0, 1)
    rows = rows.reshape(-1, rows.shape[-1])
    row_count = rows.shape[0]

    def project(matrix, widths):
        made = jnp.dot(rows, matrix, preferred_element_type=jnp.float32).astype(jnp.bfloat16)
        bounds = [sum(widths[:i]) for i in range(len(widths) + 1)]
        return [made[:, bounds[i] : bounds[i + 1]] for i in range(len(widths))]

    early = (query_weight, key_weight, value_weight, unit_value, unit_gate)
    late = (retain_gate, convolve_gate)
    late_width = sum(m.shape[1] // 2 for m in late)
    queries, key_rows, values, glu_value, glu_switch = project(
        first, [m.shape[1] // 2 for m in early]
    )
    retain_switch, convolve_switch = project(
        second[:, :late_width], [m.shape[1] // 2 for m in late]
    )
    out_full = second[:, late_width:]
    local_heads = queries.shape[1] // KEY
    positions = (chain_rank // 2) * row_count + jnp.arange(row_count, dtype=jnp.int32)
    rotated_query, rotated_keys, value_heads = prepare(queries, key_rows, values, positions)
    place = head_rank * 2 + side
    log_decay = decay_logs(
        place * local_heads,
        local_heads,
        local_heads * head_groups * 2,
        row_count * pairs_total,
    )
    within, contribution = local_parts(rotated_query, rotated_keys, value_heads, log_decay)
    totals = jnp.exp(log_decay * row_count)
    gated_input = (
        glu_value.astype(jnp.float32) * jax.nn.sigmoid(glu_switch.astype(jnp.float32))
    ).astype(jnp.bfloat16)
    channels = gated_input.shape[1]
    before = from_behind(gated_input[row_count - (KW - 1) :], "sp", 2)
    incoming = state_before(contribution, totals, "sp")
    raw = within + cross_part(rotated_query, incoming, log_decay)
    retain_hidden = retain_finish(raw, retain_switch)
    tap_slice = lax.dynamic_slice_in_dim(filter_taps, place * channels, channels, 1)
    gain_slice = lax.dynamic_slice_in_dim(layer_gain, place * channels, channels, 0)
    shift_slice = lax.dynamic_slice_in_dim(layer_shift, place * channels, channels, 0)
    convolve_hidden = convolve_branch(
        gated_input, before, tap_slice, gain_slice, shift_slice, convolve_switch
    )
    hidden = jnp.concatenate((retain_hidden, convolve_hidden), axis=1)
    return scatter_sums(lambda rows: contract(rows, out_full), hidden, "tp", "sp")


def solution(mesh):
    return jax.shard_map(
        local,
        mesh=mesh,
        in_specs=(
            P(("sp", "tp"), None),
            P(),
            P("sp", "tp"),
            P("sp", "tp"),
            P("sp", "tp"),
            P("sp", "tp"),
            P("sp", "tp"),
            P("sp", "tp"),
            P("sp", "tp"),
            P(),
            P(),
            P(),
            P("sp", "tp"),
            P("sp", "tp"),
        ),
        out_specs=P(("sp", "tp"), None),
        check_vma=False,
    )
```
